32 devices in a mesh: grp: 2 (over y), sp: 4 (over z), tp: 4 (over x, core).
Axes of the slice: x: 2, y: 2, z: 4, core: 2. Of those that a mesh axis runs over, the one named last changes fastest.
Arguments:
- latent: bfloat16 [4096, 2048], P(('grp', 'sp', 'tp')), parts along dimension 0, may hold values from -3 to 3
- context: bfloat16 [1024, 2048], P(('grp', 'sp')), parts along dimension 0, may hold values from -6 to 6
- condition: float32 [4096], P(('grp', 'sp')), parts along dimension 0, may hold values from -6 to 6
- context_condition: float32 [2048], P('sp'), may hold values from -6 to 6
- mod_weight: bfloat16 [2048, 6144], P('sp', 'tp'), may hold values from -0.1875 to 0.1875
- mod_bias: float32 [6144], replicated, may hold values from -1.5 to 1.5
- query_weight: bfloat16 [2048, 1024], P('sp'), may hold values from -0.125 to 0.125
- key_weight: bfloat16 [2048, 1024], P('sp'), may hold values from -0.125 to 0.125
- value_weight: bfloat16 [2048, 2048], P(None, 'tp'), may hold values from -3 to 3
- out_gate_weight: bfloat16 [2048, 2048], P(None, 'tp'), may hold values from -0.125 to 0.125
- decay_in_weight: bfloat16 [2048, 32], replicated, may hold values from -0.125 to 0.125
- decay_weight: bfloat16 [2, 16, 1024], replicated, may hold values from -1.5 to 1.5
- decay_bias: float32 [2, 1024], replicated, may hold values from 0.5 to 11
- extra_decay: float32 [2, 4, 2048], P(None, None, 'sp'), may hold values from -2.1 to 0
- norm_gain: float32 [512], replicated, may hold values from 0.1 to 1.9
- out_weight: bfloat16 [2048, 2048], P('tp'), may hold values from -0.25 to 0.25
- final_gain: float32 [2048], replicated, may hold values from 0.1 to 1.9
- final_bias: float32 [2048], replicated, may hold values from -1.5 to 1.5
Outputs:
- output: bfloat16 [4096, 2048], P(('grp', 'sp', 'tp')), parts along dimension 0
The draws below stay inside these ranges and needn't reach their ends.
There are 2 independent parts, one for each index of `grp`. The reference program is written for one: setup_inputs(seed, part) draws one part's arguments, and reference() takes and returns one part's arrays. A program takes and returns all parts, laid end to end along the dimension named above; an argument that names none is the same for every part. Nothing has to cross between parts.
All inputs are finite; a program needn't handle non-finite values.
Results may differ from the reference program's by a relative error of at most 0.012.
The reference program's roundings to bfloat16 on the way count: a program that leaves them out, or rounds other values in their place, can miss the bound.
Values may be sent and summed in bfloat16 or wider, within the bound.
A program may use at most 64 MiB of HBM per device.

```python
import math
import jax
import jax.numpy as jnp
from jax import lax

D = 2048
ATTENTION_HEADS = 4
DK = 256
DV = 512
RANK = 16
BLOCK = 64
GRID_W = 64
CTX = 512
TOK_SP = 512
LATENT_TOKENS = 2048
QK = 1024
VD = 2048


def draw_value_weight(key, part):
    noise = jax.random.truncated_normal(key, -4.0, 4.0, (D, ATTENTION_HEADS * DV), jnp.float32)
    column = (jnp.arange(ATTENTION_HEADS * DV) % DV).astype(jnp.float32)
    rising = 4.0 ** (column / DV)
    return (noise * rising * (0.6 / math.sqrt(D))).astype(jnp.bfloat16)


def draw_decay_bias(key, part):
    choose_key, slow_key, fast_key = jax.random.split(key, 3)
    fast_share = 0.5
    picked = jax.random.uniform(choose_key, (2, ATTENTION_HEADS * DK), jnp.float32) < fast_share
    slow_values = jax.random.uniform(slow_key, (2, ATTENTION_HEADS * DK), jnp.float32, 9.0, 11.0)
    fast_values = jax.random.uniform(fast_key, (2, ATTENTION_HEADS * DK), jnp.float32, 0.5, 2.0)
    return jnp.where(picked, fast_values, slow_values)


def draw_extra_decay(key, part):
    rate_key, location_key, keep_key = jax.random.split(key, 3)
    blocks = LATENT_TOKENS // TOK_SP
    rate_values = jnp.exp(jax.random.uniform(rate_key, (2, ATTENTION_HEADS, blocks), jnp.float32, math.log(0.15), math.log(0.9)))
    stable_part = -jnp.repeat(rate_values, TOK_SP, axis=2) / LATENT_TOKENS
    spike_locations = jax.random.randint(location_key, (2, ATTENTION_HEADS, 3), 0, LATENT_TOKENS)
    retain_fraction = jax.random.uniform(keep_key, (2, ATTENTION_HEADS, 3), jnp.float32, 0.5, 0.8)
    token_places = jnp.arange(LATENT_TOKENS)
    match_lookup = token_places[None, None, None, :] == spike_locations[:, :, :, None]
    spike_events = jnp.sum(jnp.where(match_lookup, jnp.log(retain_fraction)[:, :, :, None], 0.0), axis=2)
    return stable_part + spike_events


def steps_of(key, extent, cuts, least, high):
    def one(position, shards_of):
        heights = jax.random.uniform(jax.random.fold_in(jax.random.fold_in(key, 6), position), (shards_of,), jnp.float32, least / len(cuts), high / len(cuts))
        return jnp.repeat(jnp.exp(heights), extent[position] // shards_of).reshape((-1,) + (1,) * (len(extent) - position - 1))

    loudness = one(*cuts[0])
    for cut in cuts[1:]:
        loudness = loudness * one(*cut)
    return loudness


def gaussian(key, dims, scale, limit, pieces=(), kind=jnp.bfloat16):
    values = scale * jax.random.normal(key, dims, jnp.float32)
    if pieces:
        values = values * steps_of(key, dims, pieces, -0.22, 0.18)
    return jnp.clip(values, -limit, limit).astype(kind)


def setup_inputs(seed: int = 0, part: int = 0) -> dict:
    seeds = jax.random.split(jax.random.key(seed), 19)
    own_keys = jax.random.split(jax.random.fold_in(seeds[18], part), 19)
    return {
        "latent": gaussian(own_keys[0], (LATENT_TOKENS, D), 0.5, 3.0, ((0, 16),)),
        "context": gaussian(own_keys[1], (CTX, D), 1.0, 6.0, ((0, 4),)),
        "condition": gaussian(own_keys[2], (D,), 1.0, 6.0, ((0, 4),), jnp.float32),
        "context_condition": gaussian(seeds[3], (D,), 1.0, 6.0, ((0, 4),), jnp.float32),
        "mod_weight": gaussian(seeds[4], (D, 3 * D), (D // 2) ** -0.5, 0.1875, ((0, 4), (1, 4))),
        "mod_bias": gaussian(seeds[5], (3 * D,), 0.3, 1.5, (), jnp.float32),
        "query_weight": gaussian(seeds[6], (D, QK), D ** -0.5, 0.125, ((0, 4),)),
        "key_weight": gaussian(seeds[7], (D, QK), D ** -0.5, 0.125, ((0, 4),)),
        "value_weight": draw_value_weight(jax.random.fold_in(seeds[18], 71), part),
        "out_gate_weight": gaussian(seeds[9], (D, VD), D ** -0.5, 0.125, ((1, 4),)),
        "decay_in_weight": gaussian(seeds[10], (D, 2 * RANK), D ** -0.5, 0.125),
        "decay_weight": gaussian(seeds[11], (2, RANK, QK), RANK ** -0.5, 1.5),
        "decay_bias": draw_decay_bias(jax.random.fold_in(seeds[18], 71), part),
        "extra_decay": draw_extra_decay(jax.random.fold_in(seeds[18], 71), part),
        "norm_gain": jnp.clip(1.0 + 0.18 * jax.random.normal(seeds[14], (DV,), jnp.float32), 0.1, 1.9),
        "out_weight": gaussian(seeds[15], (VD, D), (VD // 4) ** -0.5, 0.25, ((0, 4),)),
        "final_gain": jnp.clip(1.0 + 0.18 * jax.random.normal(seeds[16], (D,), jnp.float32), 0.1, 1.9),
        "final_bias": gaussian(seeds[17], (D,), 0.3, 1.5, (), jnp.float32),
    }


norm_eps = 1e-05
gate_scale = 16.0
rope_base = 10000.0
residual_scale = 2.0 ** 0.5
highest = lax.Precision.HIGHEST

def rotate_half(values, angle):
    half_width = values.shape[-1] // 2
    first_half = values[..., :half_width]
    second_half = values[..., half_width:]
    cosine = jnp.cos(angle)
    sine_part = jnp.sin(angle)
    return jnp.concatenate([first_half * cosine - second_half * sine_part, first_half * sine_part + second_half * cosine], axis=-1)

def rotary(values, token_places):
    quarter = values.shape[-1] // 4
    frequency = rope_base ** (-jnp.arange(quarter, dtype=jnp.float32) / quarter)
    row_index = (token_places // GRID_W).astype(jnp.float32)
    col_index = (token_places % GRID_W).astype(jnp.float32)
    half_width = 2 * quarter
    by_row = rotate_half(values[..., :half_width], row_index[:, None] * frequency)
    by_col = rotate_half(values[..., half_width:], col_index[:, None] * frequency)
    return jnp.concatenate([by_row, by_col], axis=-1)

def log_decays(low_rank, decay_weight, decay_bias):
    rank_width = decay_weight.shape[1]
    decay_parts = []
    for direction in range(2):
        logits = jnp.dot(low_rank[:, direction * rank_width:(direction + 1) * rank_width], decay_weight[direction], preferred_element_type=jnp.float32) + decay_bias[direction]
        decay_parts.append(jax.nn.log_sigmoid(logits) / gate_scale)
    return decay_parts

def by_head(rows, size):
    return rows.astype(jnp.float32).reshape(rows.shape[0], -1, size).transpose(1, 0, 2)

def flip_rows(values):
    return jnp.flip(values, axis=1)

def end_state(key_heads, value_heads, logdec):
    cumulative = jnp.cumsum(logdec, axis=1)
    weights = jnp.exp(cumulative[:, -1:] - cumulative)
    return jnp.einsum('hnd,hnv->hdv', key_heads * weights, value_heads, precision=highest)

def blocked_scan(queries, key_heads, value_heads, logdec, start):
    heads, length, unused_width = queries.shape
    block_count = length // BLOCK
    lower_mask = jnp.tril(jnp.ones((BLOCK, BLOCK), dtype=bool))

    def blocks(values):
        return jnp.moveaxis(values.reshape(heads, block_count, BLOCK, values.shape[-1]), 1, 0)

    def advance(carry_state, block_data):
        query_block, key_block, value_block, decay_block = block_data
        cumulative = jnp.cumsum(decay_block, axis=1)
        total_decay = cumulative[:, -1:]
        query_decayed = query_block * jnp.exp(cumulative)
        key_inverse = key_block * jnp.exp(-cumulative)
        key_closing = key_block * jnp.exp(total_decay - cumulative)
        scores = jnp.einsum('hcd,hsd->hcs', query_decayed, key_inverse, precision=highest)
        scores = jnp.where(lower_mask[None], scores, 0.0)
        outputs = jnp.einsum('hcs,hsv->hcv', scores, value_block, precision=highest) + jnp.einsum('hcd,hdv->hcv', query_decayed, carry_state, precision=highest)
        carry_state = jnp.exp(total_decay)[:, 0, :, None] * carry_state + jnp.einsum('hcd,hcv->hdv', key_closing, value_block, precision=highest)
        return (carry_state, outputs)
    unused_state, outputs = lax.scan(advance, start, (blocks(queries), blocks(key_heads), blocks(value_heads), blocks(logdec)))
    return jnp.moveaxis(outputs, 0, 1).reshape(heads, length, value_heads.shape[-1])

def reference(latent, context, condition, context_condition, mod_weight, mod_bias, query_weight, key_weight, value_weight, out_gate_weight, decay_in_weight, decay_weight, decay_bias, extra_decay, norm_gain, out_weight, final_gain, final_bias):
    model_width = latent.shape[1]
    activated = jax.nn.silu(jnp.stack([condition, context_condition])).astype(jnp.bfloat16)
    modulation = jnp.dot(activated, mod_weight, preferred_element_type=jnp.float32) + mod_bias
    shifts = modulation[:, :model_width]
    scales = modulation[:, model_width:2 * model_width]
    branch_gate = modulation[0, 2 * model_width:]
    mod_latent = (latent.astype(jnp.float32) * (1.0 + scales[0]) + shifts[0]).astype(jnp.bfloat16)
    mod_context = (context.astype(jnp.float32) * (1.0 + scales[1]) + shifts[1]).astype(jnp.bfloat16)

    def project(rows, weight):
        return jnp.dot(rows, weight, preferred_element_type=jnp.float32).astype(jnp.bfloat16)
    queries = project(mod_latent, query_weight)
    out_gate = project(mod_latent, out_gate_weight)
    key_rows = project(mod_latent, key_weight)
    value_rows = project(mod_latent, value_weight)
    low_rank = project(mod_latent, decay_in_weight)
    context_keys = project(mod_context, key_weight)
    context_values = project(mod_context, value_weight)
    context_low = project(mod_context, decay_in_weight)
    token_places = jnp.arange(LATENT_TOKENS, dtype=jnp.int32)
    query_heads = rotary(by_head(queries, DK) * DK ** (-0.5), token_places)
    key_heads = rotary(by_head(key_rows, DK), token_places)
    value_heads = by_head(value_rows, DV)
    latent_decay = log_decays(low_rank, decay_weight, decay_bias)
    forward_decay = by_head(latent_decay[0], DK) + extra_decay[0][:, :, None]
    backward_decay = by_head(latent_decay[1], DK) + extra_decay[1][:, :, None]
    context_decay = log_decays(context_low, decay_weight, decay_bias)
    ctx_key_heads = by_head(context_keys, DK)
    ctx_value_heads = by_head(context_values, DV)
    start_forward = end_state(ctx_key_heads, ctx_value_heads, by_head(context_decay[0], DK))
    start_backward = end_state(flip_rows(ctx_key_heads), flip_rows(ctx_value_heads), flip_rows(by_head(context_decay[1], DK)))
    out_forward = blocked_scan(query_heads, key_heads, value_heads, forward_decay, start_forward)
    out_backward = flip_rows(blocked_scan(flip_rows(query_heads), flip_rows(key_heads), flip_rows(value_heads), flip_rows(backward_decay), start_backward))
    mixture = out_forward + out_backward
    normed = mixture * lax.rsqrt(lax.optimization_barrier(jnp.mean(mixture * mixture, axis=-1, keepdims=True)) + norm_eps) * norm_gain
    normed = normed.transpose(1, 0, 2).reshape(LATENT_TOKENS, ATTENTION_HEADS * DV)
    gated_rows = (normed * jax.nn.silu(out_gate.astype(jnp.float32))).astype(jnp.bfloat16)
    branch = jnp.dot(gated_rows, out_weight, preferred_element_type=jnp.float32)
    summed = residual_scale * latent.astype(jnp.float32) + branch_gate * branch
    row_mean = lax.optimization_barrier(jnp.mean(summed, axis=1, keepdims=True))
    centered = summed - row_mean
    variance = lax.optimization_barrier(jnp.mean(centered * centered, axis=1, keepdims=True))
    return (centered * lax.rsqrt(variance + norm_eps) * final_gain + final_bias).astype(jnp.bfloat16)
```

```python
import functools

import jax
import jax.numpy as jnp
from jax import lax
from jax.experimental import pallas as pl
from jax.experimental.pallas import tpu as pltpu
from jax.sharding import PartitionSpec as P

ATTENTION_HEADS = 4
DV = 512
BLOCK = 64
GRID_W = 64


norm_eps = 1e-05
gate_scale = 16.0
rope_base = 10000.0
residual_scale = 2.0**0.5
highest = lax.Precision.HIGHEST
f32 = jnp.float32
bf16 = jnp.bfloat16


def rope_tables(token_places, width):
    quarter = width // 4
    frequency = rope_base ** (-jnp.arange(quarter, dtype=f32) / quarter)
    row_angle = (token_places // GRID_W).astype(f32)[:, None] * frequency
    col_angle = (token_places % GRID_W).astype(f32)[:, None] * frequency
    cosine = jnp.concatenate([jnp.cos(row_angle)] * 2 + [jnp.cos(col_angle)] * 2, axis=1)
    row_sine, col_sine = jnp.sin(row_angle), jnp.sin(col_angle)
    sine = jnp.concatenate([-row_sine, row_sine, -col_sine, col_sine], axis=1)
    return cosine, sine


def dot(a, b, contract=((1,), (0,)), precision=None):
    return lax.dot_general(a, b, (contract, ((), ())), precision=precision,
                           preferred_element_type=f32)


def log_sigmoid(x):
    return jnp.minimum(x, 0.0) - jnp.log1p(jnp.exp(-jnp.abs(x)))


def rotate(x, cosine, sine):
    half = x.shape[1] // 2
    parts = [pltpu.roll(x[:, i * half:(i + 1) * half], half // 2, 1) for i in range(2)]
    return x * cosine + jnp.concatenate(parts, axis=1) * sine


def triangle(size, reverse):
    row = lax.broadcasted_iota(jnp.int32, (size, size), 0)
    col = lax.broadcasted_iota(jnp.int32, (size, size), 1)
    return row <= col if reverse else row >= col


def decay_block(low, decay_weight, decay_bias, direction):
    rank = decay_weight.shape[1]
    logits = dot(low[:, direction * rank:(direction + 1) * rank], decay_weight[direction])
    return log_sigmoid(logits + decay_bias[direction:direction + 1, :]) / gate_scale


def context_kernel(k_ref, v_ref, low_ref, dw_ref, db_ref, state_ref):
    length, width = k_ref.shape
    size = min(2 * BLOCK, length)
    count = length // size
    for direction in range(2):
        mask = triangle(size, direction == 1).astype(f32)
        edge = 0 if direction == 1 else size - 1
        state = None
        for step in range(count):
            b = count - 1 - step if direction == 1 else step
            rows = slice(b * size, (b + 1) * size)
            logdec = decay_block(low_ref[rows, :], dw_ref[...], db_ref[...], direction)
            cum = dot(mask, logdec, precision=highest)
            total = cum[edge:edge + 1, :]
            closing = (k_ref[rows, :].astype(f32) * jnp.exp(total - cum)).astype(bf16)
            term = dot(closing, v_ref[rows, :], ((0,), (0,)))
            state = term if state is None else jnp.exp(total).T * state + term
        state_ref[direction] = state


def local_kernel(q_ref, k_ref, v_ref, low_ref, extra_ref, dw_ref, db_ref, cos_ref, sin_ref,
                 out_ref, qc_ref, state_ref, total_ref):
    length, width = q_ref.shape
    size = 2 * BLOCK
    count = length // size
    rq, rk, within, scores = [], [], [], []
    for b in range(count):
        rows = slice(b * size, (b + 1) * size)
        cosine, sine = cos_ref[rows, :], sin_ref[rows, :]
        rq.append(rotate(q_ref[rows, :].astype(f32) * width ** -0.5, cosine, sine))
        rk.append(rotate(k_ref[rows, :].astype(f32), cosine, sine))
        scores.append(None)
    for direction in range(2):
        keep = triangle(size, direction == 1)
        mask = keep.astype(f32)
        edge = 0 if direction == 1 else size - 1
        middle = size // 2 if direction == 1 else size // 2 - 1
        state = None
        before = None
        for step in range(count):
            b = count - 1 - step if direction == 1 else step
            rows = slice(b * size, (b + 1) * size)
            logdec = decay_block(low_ref[rows, :], dw_ref[...], db_ref[...], direction)
            logdec = logdec + extra_ref[rows, direction:direction + 1]
            cum = dot(mask, logdec, precision=highest)
            total = cum[edge:edge + 1, :]
            center = cum[middle:middle + 1, :]
            q_mid = (rq[b] * jnp.exp(cum - center)).astype(bf16)
            k_mid = (rk[b] * jnp.exp(center - cum)).astype(bf16)
            score = jnp.where(keep, dot(q_mid, k_mid, ((1,), (1,))), 0.0)
            q_dec = rq[b] * jnp.exp(cum)
            if direction == 0:
                scores[b] = score
                out = None
            else:
                out = dot((scores[b] + score).astype(bf16), v_ref[rows, :])
            if state is not None:
                carried = dot(q_dec.astype(bf16), state.astype(bf16))
                out = carried if out is None else out + carried
            if direction == 0:
                out_ref[rows, :] = jnp.zeros((size, v_ref.shape[1]), f32) if out is None else out
            else:
                out_ref[rows, :] += out
            q_all = q_dec if before is None else q_dec * jnp.exp(before)
            qc_ref[rows, direction * width:(direction + 1) * width] = q_all.astype(bf16)
            closing = (rk[b] * jnp.exp(total - cum)).astype(bf16)
            term = dot(closing, v_ref[rows, :], ((0,), (0,)))
            state = term if state is None else jnp.exp(total).T * state + term
            before = total if before is None else before + total
        state_ref[direction * width:(direction + 1) * width, :] = state.astype(bf16)
        total_ref[direction:direction + 1, :] = before


def join_kernel(final, out_ref, qc_ref, states_ref, totals_ref, start_ref, gate_ref, gain_ref,
                place_ref, result_ref):
    count = states_ref.shape[0]
    width = qc_ref.shape[1] // 2
    place = place_ref[...]
    mixture = out_ref[...]
    for direction in range(2):
        state = start_ref[direction]
        for lap in range(count):
            j = count - 1 - lap if direction == 1 else lap
            decay = jnp.exp(totals_ref[j, direction:direction + 1, :]).T
            joined = decay * state + states_ref[
                j, direction * width:(direction + 1) * width, :].astype(f32)
            ahead = place < j if direction == 1 else place > j
            state = jnp.where(ahead, joined, state)
        mixture = mixture + dot(qc_ref[:, direction * width:(direction + 1) * width],
                                state.astype(bf16))
    if final:
        squares = jnp.mean(mixture * mixture, axis=1, keepdims=True)
        gate = gate_ref[...].astype(f32)
        normed = mixture * lax.rsqrt(squares + norm_eps) * gain_ref[...]
        result_ref[...] = (normed * (gate / (1.0 + jnp.exp(-gate)))).astype(bf16)
    else:
        result_ref[...] = mixture


def call(kernel, out_shape, *args):
    return pl.pallas_call(
        kernel,
        out_shape=out_shape,
        in_specs=[pl.BlockSpec(memory_space=pltpu.VMEM)] * len(args),
        out_specs=jax.tree.map(lambda _: pl.BlockSpec(memory_space=pltpu.VMEM), out_shape),
        compiler_params=pltpu.CompilerParams(vmem_limit_bytes=48 * 1024 * 1024),
        cost_estimate=pl.CostEstimate(flops=4_000_000_000, bytes_accessed=4_000_000,
                                      transcendentals=1_000_000),
    )(*args)


def project(rows, weight):
    return jnp.dot(rows, weight, preferred_element_type=f32).astype(bf16)


def body(
    latent,
    context,
    condition,
    context_condition,
    mod_weight,
    mod_bias,
    query_weight,
    key_weight,
    value_weight,
    out_gate_weight,
    decay_in_weight,
    decay_weight,
    decay_bias,
    extra_decay,
    norm_gain,
    out_weight,
    final_gain,
    final_bias,
):
    model_width = latent.shape[1]
    head_keys = query_weight.shape[1] // ATTENTION_HEADS
    value_cols = value_weight.shape[1]
    tp_index = lax.axis_index("tp")
    sp_index = lax.axis_index("sp")
    head_share = lax.axis_size("tp") // ATTENTION_HEADS
    head_index = tp_index // head_share
    part_index = tp_index % head_share
    key_start = head_index * head_keys

    own_qk = jnp.concatenate(
        [lax.dynamic_slice_in_dim(w, key_start, head_keys, 1) for w in (query_weight, key_weight)],
        axis=1,
    )
    activated = jax.nn.silu(jnp.stack([condition, context_condition])).astype(bf16)
    partial_value = jnp.dot(activated, mod_weight, preferred_element_type=f32)
    row_sums = lax.psum(partial_value, "sp")
    modulation = lax.all_gather(row_sums, "tp", axis=1, tiled=True)
    modulation = modulation + mod_bias
    shifts = modulation[:, :model_width]
    scales = modulation[:, model_width : 2 * model_width]
    branch_gate = modulation[0, 2 * model_width :]

    qk_head = lax.all_gather(own_qk, "sp", axis=0, tiled=True)
    rows = lax.all_gather(latent, "tp", axis=0, tiled=True)
    mod_context = (context.astype(f32) * (1.0 + scales[1]) + shifts[1]).astype(bf16)
    context_local = jnp.concatenate(
        [
            project(mod_context, qk_head[:, head_keys:]),
            project(mod_context, value_weight),
            project(mod_context, decay_in_weight),
        ],
        axis=1,
    )
    gathered_context = lax.all_gather(context_local, "sp", axis=0, tiled=True)
    mod_latent = (rows.astype(f32) * (1.0 + scales[0]) + shifts[0]).astype(bf16)
    qk = project(mod_latent, qk_head)
    value_rows = project(mod_latent, value_weight)
    out_gate = project(mod_latent, out_gate_weight)
    low_rank = project(mod_latent, decay_in_weight)
    count = rows.shape[0]
    token_places = sp_index * count + jnp.arange(count, dtype=jnp.int32)
    cosine, sine = rope_tables(token_places, head_keys)
    head_bias = lax.dynamic_slice_in_dim(decay_bias, key_start, head_keys, 1)
    head_gate = lax.dynamic_slice_in_dim(decay_weight, key_start, head_keys, 2)
    head_extra = lax.dynamic_index_in_dim(extra_decay, head_index, 1, keepdims=False).T

    sds = jax.ShapeDtypeStruct
    out_local, qc, states, totals = call(
        local_kernel,
        (
            sds((count, value_cols), f32),
            sds((count, 2 * head_keys), bf16),
            sds((2 * head_keys, value_cols), bf16),
            sds((2, head_keys), f32),
        ),
        qk[:, :head_keys], qk[:, head_keys:], value_rows, low_rank, head_extra, head_gate,
        head_bias, cosine, sine,
    )
    start = call(
        context_kernel,
        sds((2, head_keys, value_cols), f32),
        gathered_context[:, :head_keys],
        gathered_context[:, head_keys : head_keys + value_cols],
        gathered_context[:, head_keys + value_cols :],
        head_gate, head_bias,
    )
    all_states = lax.all_gather(states, "sp")
    all_totals = lax.all_gather(totals, "sp")
    place = jnp.full((1, value_cols), sp_index, jnp.int32)
    gain_slice = lax.dynamic_slice_in_dim(norm_gain, part_index * value_cols, value_cols, 0)
    final = head_share == 1
    joined = call(
        functools.partial(join_kernel, final),
        sds((count, value_cols), bf16 if final else f32),
        out_local, qc, all_states, all_totals, start, out_gate, gain_slice[None, :], place,
    )
    if final:
        gated_rows = joined
    else:
        squares = jnp.sum(joined * joined, axis=1)
        onehot = (jnp.arange(ATTENTION_HEADS) == head_index).astype(f32)
        sums = lax.psum(onehot[:, None] * squares[None, :], "tp")
        head_sum = jnp.sum(sums * onehot[:, None], axis=0)
        normed = joined * lax.rsqrt(head_sum / DV + norm_eps)[:, None] * gain_slice
        gated_rows = (normed * jax.nn.silu(out_gate.astype(f32))).astype(bf16)
    full_out = lax.all_gather(out_weight, "tp", axis=0, tiled=True)
    regrouped = lax.all_to_all(gated_rows, "tp", split_axis=0, concat_axis=1, tiled=True)
    branch = jnp.dot(regrouped, full_out, preferred_element_type=f32)
    summed = residual_scale * latent.astype(f32) + branch_gate * branch
    row_mean = jnp.mean(summed, axis=1, keepdims=True)
    centered = summed - row_mean
    variance = jnp.mean(centered * centered, axis=1, keepdims=True)
    return (centered * lax.rsqrt(variance + norm_eps) * final_gain + final_bias).astype(bf16)


def solution(mesh):
    placed = (
        P(("grp", "sp", "tp"), None),
        P(("grp", "sp"), None),
        P(("grp", "sp")),
        P("sp"),
        P("sp", "tp"),
        P(),
        P("sp", None),
        P("sp", None),
        P(None, "tp"),
        P(None, "tp"),
        P(),
        P(),
        P(),
        P(None, None, "sp"),
        P(),
        P("tp", None),
        P(),
        P(),
    )
    return jax.shard_map(
        body, mesh=mesh, in_specs=placed, out_specs=P(("grp", "sp", "tp"), None), check_vma=False
    )
```

```python
import functools

import jax
import jax.numpy as jnp
from jax import lax
from jax.experimental import pallas as pl
from jax.experimental.pallas import tpu as pltpu
from jax.sharding import PartitionSpec as P

ATTENTION_HEADS = 4
DV = 512
BLOCK = 64
GRID_W = 64


norm_eps = 1e-05
gate_scale = 16.0
rope_base = 10000.0
residual_scale = 2.0**0.5
highest = lax.Precision.HIGHEST
f32 = jnp.float32
bf16 = jnp.bfloat16


def rope_tables(token_places, width):
    quarter = width // 4
    frequency = rope_base ** (-jnp.arange(quarter, dtype=f32) / quarter)
    row_angle = (token_places // GRID_W).astype(f32)[:, None] * frequency
    col_angle = (token_places % GRID_W).astype(f32)[:, None] * frequency
    cosine = jnp.concatenate([jnp.cos(row_angle)] * 2 + [jnp.cos(col_angle)] * 2, axis=1)
    row_sine, col_sine = jnp.sin(row_angle), jnp.sin(col_angle)
    sine = jnp.concatenate([-row_sine, row_sine, -col_sine, col_sine], axis=1)
    return cosine, sine


def dot(a, b, contract=((1,), (0,)), precision=None):
    return lax.dot_general(a, b, (contract, ((), ())), precision=precision,
                           preferred_element_type=f32)


def log_sigmoid(x):
    return jnp.minimum(x, 0.0) - jnp.log1p(jnp.exp(-jnp.abs(x)))


def rotate(x, cosine, sine):
    half = x.shape[1] // 2
    parts = [pltpu.roll(x[:, i * half:(i + 1) * half], half // 2, 1) for i in range(2)]
    return x * cosine + jnp.concatenate(parts, axis=1) * sine


def triangle(size, reverse):
    row = lax.broadcasted_iota(jnp.int32, (size, size), 0)
    col = lax.broadcasted_iota(jnp.int32, (size, size), 1)
    return row <= col if reverse else row >= col


def decay_block(low, decay_weight, decay_bias, direction):
    rank = decay_weight.shape[1]
    logits = dot(low[:, direction * rank:(direction + 1) * rank], decay_weight[direction])
    return log_sigmoid(logits + decay_bias[direction:direction + 1, :]) / gate_scale


def context_kernel(k_ref, v_ref, low_ref, dw_ref, db_ref, state_ref):
    length, width = k_ref.shape
    size = min(2 * BLOCK, length)
    count = length // size
    for direction in range(2):
        mask = triangle(size, direction == 1).astype(f32)
        edge = 0 if direction == 1 else size - 1
        state = None
        for step in range(count):
            b = count - 1 - step if direction == 1 else step
            rows = slice(b * size, (b + 1) * size)
            logdec = decay_block(low_ref[rows, :], dw_ref[...], db_ref[...], direction)
            cum = dot(mask, logdec, precision=highest)
            total = cum[edge:edge + 1, :]
            closing = (k_ref[rows, :].astype(f32) * jnp.exp(total - cum)).astype(bf16)
            term = dot(closing, v_ref[rows, :], ((0,), (0,)))
            state = term if state is None else jnp.exp(total).T * state + term
        state_ref[direction] = state


def local_kernel(q_ref, k_ref, v_ref, low_ref, extra_ref, dw_ref, db_ref, cos_ref, sin_ref,
                 out_ref, qc_ref, state_ref, total_ref):
    length, width = q_ref.shape
    size = 2 * BLOCK
    count = length // size
    rq, rk, within, scores = [], [], [], []
    for b in range(count):
        rows = slice(b * size, (b + 1) * size)
        cosine, sine = cos_ref[rows, :], sin_ref[rows, :]
        rq.append(rotate(q_ref[rows, :].astype(f32) * width ** -0.5, cosine, sine))
        rk.append(rotate(k_ref[rows, :].astype(f32), cosine, sine))
        scores.append(None)
    for direction in range(2):
        keep = triangle(size, direction == 1)
        mask = keep.astype(f32)
        edge = 0 if direction == 1 else size - 1
        middle = size // 2 if direction == 1 else size // 2 - 1
        state = None
        before = None
        for step in range(count):
            b = count - 1 - step if direction == 1 else step
            rows = slice(b * size, (b + 1) * size)
            logdec = decay_block(low_ref[rows, :], dw_ref[...], db_ref[...], direction)
            logdec = logdec + extra_ref[rows, direction:direction + 1]
            cum = dot(mask, logdec, precision=highest)
            total = cum[edge:edge + 1, :]
            center = cum[middle:middle + 1, :]
            q_mid = (rq[b] * jnp.exp(cum - center)).astype(bf16)
            k_mid = (rk[b] * jnp.exp(center - cum)).astype(bf16)
            score = jnp.where(keep, dot(q_mid, k_mid, ((1,), (1,))), 0.0)
            q_dec = rq[b] * jnp.exp(cum)
            if direction == 0:
                scores[b] = score
                out = None
            else:
                out = dot((scores[b] + score).astype(bf16), v_ref[rows, :])
            if state is not None:
                carried = dot(q_dec.astype(bf16), state.astype(bf16))
                out = carried if out is None else out + carried
            if direction == 0:
                out_ref[rows, :] = jnp.zeros((size, v_ref.shape[1]), f32) if out is None else out
            else:
                out_ref[rows, :] += out
            q_all = q_dec if before is None else q_dec * jnp.exp(before)
            qc_ref[rows, direction * width:(direction + 1) * width] = q_all.astype(bf16)
            closing = (rk[b] * jnp.exp(total - cum)).astype(bf16)
            term = dot(closing, v_ref[rows, :], ((0,), (0,)))
            state = term if state is None else jnp.exp(total).T * state + term
            before = total if before is None else before + total
        state_ref[direction * width:(direction + 1) * width, :] = state.astype(bf16)
        total_ref[direction:direction + 1, :] = before


def join_kernel(final, out_ref, qc_ref, states_ref, totals_ref, start_ref, gate_ref, gain_ref,
                place_ref, result_ref):
    count = states_ref.shape[0]
    width = qc_ref.shape[1] // 2
    place = place_ref[...]
    mixture = out_ref[...]
    for direction in range(2):
        state = start_ref[direction]
        for lap in range(count):
            j = count - 1 - lap if direction == 1 else lap
            decay = jnp.exp(totals_ref[j, direction:direction + 1, :]).T
            joined = decay * state + states_ref[
                j, direction * width:(direction + 1) * width, :].astype(f32)
            ahead = place < j if direction == 1 else place > j
            state = jnp.where(ahead, joined, state)
        mixture = mixture + dot(qc_ref[:, direction * width:(direction + 1) * width],
                                state.astype(bf16))
    if final:
        squares = jnp.mean(mixture * mixture, axis=1, keepdims=True)
        gate = gate_ref[...].astype(f32)
        normed = mixture * lax.rsqrt(squares + norm_eps) * gain_ref[...]
        result_ref[...] = (normed * (gate / (1.0 + jnp.exp(-gate)))).astype(bf16)
    else:
        result_ref[...] = mixture


def call(kernel, out_shape, *args):
    return pl.pallas_call(
        kernel,
        out_shape=out_shape,
        in_specs=[pl.BlockSpec(memory_space=pltpu.VMEM)] * len(args),
        out_specs=jax.tree.map(lambda _: pl.BlockSpec(memory_space=pltpu.VMEM), out_shape),
        compiler_params=pltpu.CompilerParams(vmem_limit_bytes=48 * 1024 * 1024),
        cost_estimate=pl.CostEstimate(flops=4_000_000_000, bytes_accessed=4_000_000,
                                      transcendentals=1_000_000),
    )(*args)


MESH = pl.DeviceIdType.MESH


def remote(src, dst, send_sem, recv_sem, axis, target):
    return pltpu.make_async_remote_copy(
        src_ref=src, dst_ref=dst, send_sem=send_sem, recv_sem=recv_sem,
        device_id={axis: target}, device_id_type=MESH)


class Line:
    def __init__(self, place, count, axis, target_of, view, chunks, send_sem, recv_sem):
        self.place, self.count, self.axis, self.target_of = place, count, axis, target_of
        self.view, self.chunks, self.send_sem, self.recv_sem = view, chunks, send_sem, recv_sem

    def copy(self, way, hop, chunk, block, target):
        ref = self.view(block, chunk)
        return remote(ref, ref, self.send_sem.at[way, hop, chunk],
                      self.recv_sem.at[way, hop, chunk], self.axis, self.target_of(target))

    def outgoing(self, way, hop):
        place, count = self.place, self.count
        if way == 0:
            return place - hop, place + 1, jnp.logical_and(place >= hop, place < count - 1)
        return place + hop, place - 1, jnp.logical_and(place + hop < count, place > 0)

    def each_send(self, way, hop, chunk, act):
        block, target, valid = self.outgoing(way, hop)

        @pl.when(valid)
        def _():
            act(self.copy(way, hop, chunk, block, target))

    def send(self, way, hop, chunk):
        self.each_send(way, hop, chunk, lambda c: c.start())

    def drain(self):
        for way in range(2):
            for hop in range(self.count - 1):
                for chunk in range(self.chunks):
                    self.each_send(way, hop, chunk, lambda c: c.wait_send())

    def arrive(self, way, hop, chunk, then=None):
        if way == 0:
            block, source, valid = self.place - 1 - hop, self.place - 1, self.place > hop
        else:
            block, source = self.place + 1 + hop, self.place + 1
            valid = self.place + 1 + hop < self.count

        @pl.when(valid)
        def _():
            self.copy(way, hop, chunk, block, source).wait_recv()
            if then is not None:
                then(block)

    def forward(self, hop, then=None):
        for chunk in range(self.chunks):
            for way in range(2):
                self.arrive(way, hop, chunk, None if then is None else functools.partial(then, way))
                if hop + 1 < self.count - 1:
                    self.send(way, hop + 1, chunk)


def open_kernel(partners):
    barrier = pltpu.get_barrier_semaphore()
    for axis, target in partners:
        pl.semaphore_signal(barrier, inc=1, device_id={axis: target}, device_id_type=MESH)
    return lambda: pl.semaphore_wait(barrier, len(partners))


def others(axis):
    count, place = lax.axis_size(axis), lax.axis_index(axis)
    return [lax.rem(place + k, count) for k in range(1, count)]


def sources(axis):
    count, place = lax.axis_size(axis), lax.axis_index(axis)
    return [lax.rem(place + count - k, count) for k in range(1, count)]


def spread(buffer, axis, send_sem, recv_sem):
    place = lax.axis_index(axis)
    for k, target in enumerate(others(axis)):
        remote(buffer.at[place], buffer.at[place], send_sem.at[k], recv_sem.at[k],
               axis, target).start()


def spread_arrive(buffer, axis, send_sem, recv_sem):
    for k, source in enumerate(sources(axis)):
        remote(buffer.at[source], buffer.at[source], send_sem.at[k], recv_sem.at[k],
               axis, source).wait_recv()


def spread_drain(buffer, axis, send_sem, recv_sem):
    place = lax.axis_index(axis)
    for k, target in enumerate(others(axis)):
        remote(buffer.at[place], buffer.at[place], send_sem.at[k], recv_sem.at[k],
               axis, target).wait_send()


def enter_kernel(chunks, latent_ref, context_ref, cond_ref, mw_ref, mb_ref, qw_ref, kw_ref,
                 ml_ref, mc_ref, gate_ref, qk_ref,
                 rows_ref, part_ref, sums_ref, zs, zr, xs, xr, cs, cr, ps, pr, ss, sr):
    sp, sp_count = lax.axis_index("sp"), lax.axis_size("sp")
    tp, tp_count = lax.axis_index("tp"), lax.axis_size("tp")
    own, model_width = latent_ref.shape
    depth = qw_ref.shape[0]
    head_keys = qk_ref.shape[1] // 2
    ready = open_kernel([("sp", t) for t in others("sp")] + [("tp", t) for t in others("tp")])
    v = cond_ref[...]
    activated = (v / (1.0 + jnp.exp(-v))).astype(bf16)
    part_ref[sp] = dot(activated, mw_ref[...])
    columns = pl.ds(pl.multiple_of((tp // (tp_count // ATTENTION_HEADS)) * head_keys, head_keys),
                    head_keys)
    qk_rows = pl.ds(pl.multiple_of(sp * depth, depth), depth)
    qk_ref[qk_rows, :head_keys] = qw_ref[:, columns]
    qk_ref[qk_rows, head_keys:] = kw_ref[:, columns]
    rows_ref[pl.ds(pl.multiple_of(tp * own, own), own), :] = latent_ref[...]

    step = depth // chunks
    z_line = Line(
        sp, sp_count, "sp", lambda p: p,
        lambda block, chunk: qk_ref.at[
            pl.ds(pl.multiple_of(block * depth + chunk * step, step), step), :],
        chunks, zs, zr)
    x_count = tp_count // 2
    x, core = tp // 2, tp % 2

    def rows_of(block, chunk):
        return rows_ref.at[pl.ds(pl.multiple_of((2 * block + core) * own, own), own), :]

    x_line = Line(x, x_count, "tp", lambda p: 2 * p + core, rows_of, 1, xs, xr)
    sibling = tp + 1 - 2 * core

    def cross(block, slot, other=False):
        side = 1 - core if other else core
        ref = rows_ref.at[pl.ds(pl.multiple_of((2 * block + side) * own, own), own), :]
        return remote(ref, ref, cs.at[slot], cr.at[slot], "tp", sibling)

    def slot_of(way, hop):
        return 1 + way * (x_count - 1) + hop

    ready()
    spread(part_ref, "sp", ps, pr)
    for way in range(2):
        x_line.send(way, 0, 0)
    cross(x, 0).start()
    for chunk in range(chunks):
        for way in range(2):
            z_line.send(way, 0, chunk)
    spread_arrive(part_ref, "sp", ps, pr)
    total = part_ref[0]
    for j in range(1, sp_count):
        total = total + part_ref[j]
    sums_ref[tp] = total
    spread(sums_ref, "tp", ss, sr)
    z_line.forward(0)
    for hop in range(x_count - 1):
        x_line.forward(hop, lambda way, block, hop=hop: cross(block, slot_of(way, hop)).start())
    if sp_count > 2:
        z_line.forward(1)
    spread_arrive(sums_ref, "tp", ss, sr)
    modulation = jnp.concatenate([sums_ref[j] for j in range(tp_count)], axis=1) + mb_ref[...]
    shifts = modulation[:, :model_width]
    scales = modulation[:, model_width:2 * model_width]
    gate_ref[...] = modulation[0:1, 2 * model_width:]
    mc_ref[...] = (context_ref[...].astype(f32) * (1.0 + scales[1:2]) + shifts[1:2]).astype(bf16)

    def each_cross(act_own, act_line):
        act_own()
        for way in range(2):
            for hop in range(x_count - 1):
                block = x - 1 - hop if way == 0 else x + 1 + hop
                valid = x > hop if way == 0 else x + 1 + hop < x_count

                @pl.when(valid)
                def _():
                    act_line(block, slot_of(way, hop))

    each_cross(lambda: cross(x, 0, True).wait_recv(),
               lambda block, slot: cross(block, slot, True).wait_recv())
    for j in range(tp_count):
        rows = slice(j * own, (j + 1) * own)
        ml_ref[rows, :] = (rows_ref[rows, :].astype(f32) * (1.0 + scales[0:1])
                           + shifts[0:1]).astype(bf16)
    for hop in range(2, sp_count - 1):
        z_line.forward(hop)
    each_cross(lambda: cross(x, 0).wait_send(),
               lambda block, slot: cross(block, slot).wait_send())
    spread_drain(part_ref, "sp", ps, pr)
    spread_drain(sums_ref, "tp", ss, sr)
    x_line.drain()
    z_line.drain()


def comm_call(kernel, out_shape, scratch, collective_id, *args):
    return pl.pallas_call(
        kernel,
        out_shape=out_shape,
        in_specs=[pl.BlockSpec(memory_space=pltpu.VMEM)] * len(args),
        out_specs=jax.tree.map(lambda _: pl.BlockSpec(memory_space=pltpu.VMEM), out_shape),
        scratch_shapes=scratch,
        compiler_params=pltpu.CompilerParams(
            vmem_limit_bytes=48 * 1024 * 1024, collective_id=collective_id,
            has_side_effects=True),
        cost_estimate=pl.CostEstimate(flops=20_000_000_000, bytes_accessed=60_000_000,
                                      transcendentals=1_000_000),
    )(*args)


def enter(latent, context, cond, mod_weight, mod_bias, query_weight, key_weight):
    sp_count, tp_count = lax.axis_size("sp"), lax.axis_size("tp")
    own, model_width = latent.shape
    depth = query_weight.shape[0]
    head_keys = query_weight.shape[1] // ATTENTION_HEADS
    chunks = 4
    sds = jax.ShapeDtypeStruct
    dma = pltpu.SemaphoreType.DMA
    x_hops = tp_count // 2 - 1
    return comm_call(
        functools.partial(enter_kernel, chunks),
        (
            sds((own * tp_count, model_width), bf16),
            sds(context.shape, bf16),
            sds((1, model_width), f32),
            sds((depth * sp_count, 2 * head_keys), bf16),
        ),
        [
            pltpu.VMEM((own * tp_count, model_width), bf16),
            pltpu.VMEM((sp_count, 2, mod_weight.shape[1]), f32),
            pltpu.VMEM((tp_count, 2, mod_weight.shape[1]), f32),
            dma((2, sp_count - 1, chunks)), dma((2, sp_count - 1, chunks)),
            dma((2, x_hops, 1)), dma((2, x_hops, 1)),
            dma((1 + 2 * x_hops,)), dma((1 + 2 * x_hops,)),
            dma((sp_count - 1,)), dma((sp_count - 1,)),
            dma((tp_count - 1,)), dma((tp_count - 1,)),
        ],
        1, latent, context, cond, mod_weight, mod_bias[None, :], query_weight, key_weight,
    )


def project(rows, weight):
    return jnp.dot(rows, weight, preferred_element_type=f32).astype(bf16)


def body(
    latent,
    context,
    condition,
    context_condition,
    mod_weight,
    mod_bias,
    query_weight,
    key_weight,
    value_weight,
    out_gate_weight,
    decay_in_weight,
    decay_weight,
    decay_bias,
    extra_decay,
    norm_gain,
    out_weight,
    final_gain,
    final_bias,
):
    head_keys = query_weight.shape[1] // ATTENTION_HEADS
    value_cols = value_weight.shape[1]
    tp_index = lax.axis_index("tp")
    sp_index = lax.axis_index("sp")
    head_share = lax.axis_size("tp") // ATTENTION_HEADS
    head_index = tp_index // head_share
    part_index = tp_index % head_share
    key_start = head_index * head_keys

    full_out = lax.all_gather(out_weight, "tp", axis=0, tiled=True)
    mod_latent, mod_context, branch_gate, qk_head = enter(
        latent, context, jnp.stack([condition, context_condition]), mod_weight, mod_bias,
        query_weight, key_weight,
    )
    context_local = jnp.concatenate(
        [
            project(mod_context, qk_head[:, head_keys:]),
            project(mod_context, value_weight),
            project(mod_context, decay_in_weight),
        ],
        axis=1,
    )
    gathered_context = lax.all_gather(context_local, "sp", axis=0, tiled=True)
    qk = project(mod_latent, qk_head)
    value_rows = project(mod_latent, value_weight)
    out_gate = project(mod_latent, out_gate_weight)
    low_rank = project(mod_latent, decay_in_weight)
    count = mod_latent.shape[0]
    token_places = sp_index * count + jnp.arange(count, dtype=jnp.int32)
    cosine, sine = rope_tables(token_places, head_keys)
    head_bias = lax.dynamic_slice_in_dim(decay_bias, key_start, head_keys, 1)
    head_gate = lax.dynamic_slice_in_dim(decay_weight, key_start, head_keys, 2)
    head_extra = lax.dynamic_index_in_dim(extra_decay, head_index, 1, keepdims=False).T

    sds = jax.ShapeDtypeStruct
    out_local, qc, states, totals = call(
        local_kernel,
        (
            sds((count, value_cols), f32),
            sds((count, 2 * head_keys), bf16),
            sds((2 * head_keys, value_cols), bf16),
            sds((2, head_keys), f32),
        ),
        qk[:, :head_keys], qk[:, head_keys:], value_rows, low_rank, head_extra, head_gate,
        head_bias, cosine, sine,
    )
    start = call(
        context_kernel,
        sds((2, head_keys, value_cols), f32),
        gathered_context[:, :head_keys],
        gathered_context[:, head_keys : head_keys + value_cols],
        gathered_context[:, head_keys + value_cols :],
        head_gate, head_bias,
    )
    states, totals, full_out = lax.optimization_barrier((states, totals, full_out))
    all_states = lax.all_gather(states, "sp")
    all_totals = lax.all_gather(totals, "sp")
    place = jnp.full((1, value_cols), sp_index, jnp.int32)
    gain_slice = lax.dynamic_slice_in_dim(norm_gain, part_index * value_cols, value_cols, 0)
    final = head_share == 1
    joined = call(
        functools.partial(join_kernel, final),
        sds((count, value_cols), bf16 if final else f32),
        out_local, qc, all_states, all_totals, start, out_gate, gain_slice[None, :], place,
    )
    if final:
        gated_rows = joined
    else:
        squares = jnp.sum(joined * joined, axis=1)
        onehot = (jnp.arange(ATTENTION_HEADS) == head_index).astype(f32)
        sums = lax.psum(onehot[:, None] * squares[None, :], "tp")
        head_sum = jnp.sum(sums * onehot[:, None], axis=0)
        normed = joined * lax.rsqrt(head_sum / DV + norm_eps)[:, None] * gain_slice
        gated_rows = (normed * jax.nn.silu(out_gate.astype(f32))).astype(bf16)
    regrouped = lax.all_to_all(gated_rows, "tp", split_axis=0, concat_axis=1, tiled=True)
    branch = jnp.dot(regrouped, full_out, preferred_element_type=f32)
    summed = residual_scale * latent.astype(f32) + branch_gate * branch
    row_mean = jnp.mean(summed, axis=1, keepdims=True)
    centered = summed - row_mean
    variance = jnp.mean(centered * centered, axis=1, keepdims=True)
    return (centered * lax.rsqrt(variance + norm_eps) * final_gain + final_bias).astype(bf16)


def solution(mesh):
    placed = (
        P(("grp", "sp", "tp"), None),
        P(("grp", "sp"), None),
        P(("grp", "sp")),
        P("sp"),
        P("sp", "tp"),
        P(),
        P("sp", None),
        P("sp", None),
        P(None, "tp"),
        P(None, "tp"),
        P(),
        P(),
        P(),
        P(None, None, "sp"),
        P(),
        P("tp", None),
        P(),
        P(),
    )
    return jax.shard_map(
        body, mesh=mesh, in_specs=placed, out_specs=P(("grp", "sp", "tp"), None), check_vma=False
    )
```
